32 devices in a mesh: fs: 8 (over z, y), tp: 4 (over x, core).
Axes of the slice: x: 2, y: 2, z: 4, core: 2. Of those that a mesh axis runs over, the one named last changes fastest.
Arguments:
- inputs: bfloat16 [2048, 2048], P('fs', 'tp'), may hold values from -6 to 6
- cotangent: bfloat16 [2048, 2048], P('fs', 'tp'), may hold values from -8 to 8
- gate_weight: bfloat16 [2048, 5632], P('fs', 'tp'), may hold values from -0.125 to 0.125
- up_weight: bfloat16 [2048, 5632], P('fs', 'tp'), may hold values from -0.125 to 0.125
- down_weight: bfloat16 [5632, 2048], P('tp', 'fs'), may hold values from -0.078125 to 0.078125
Outputs:
- grad_inputs: bfloat16 [2048, 2048], P('fs', 'tp')
- grad_gate: float32 [2048, 5632], P('fs', 'tp')
- grad_up: float32 [2048, 5632], P('fs', 'tp')
- grad_down: float32 [5632, 2048], P('tp', 'fs')
The draws below stay inside these ranges and needn't reach their ends.
All inputs are finite; a program needn't handle non-finite values.
Results may differ from the reference program's by a relative error of at most 0.015.
Values may be sent and summed in bfloat16 or wider, within the bound.
A program may use at most 64 MiB of HBM per device.

```python
import jax
import jax.numpy as jnp
from jax import lax

D = 2048
FF = 5632
TOKENS = 2048
N_TP = 4


def spiked(entries, own_key, source, target, blocks, factor):
    def block_of(axis_at):
        return (jnp.arange(entries.shape[axis_at]) // (entries.shape[axis_at] // blocks)).reshape((-1,) + (1,) * (entries.ndim - 1 - axis_at))

    near = jax.random.permutation(own_key, blocks)[block_of(target)]
    other_side = (block_of(target) + blocks // 2) % blocks
    return jnp.where((block_of(source) == near) | (block_of(source) == other_side), factor * entries, entries)


def levels(key, dims, cuts, smallest, high):
    level = 1.0
    for dim, blocks in cuts:
        steps = jax.random.uniform(jax.random.fold_in(jax.random.fold_in(key, 6), dim), (blocks,), jnp.float32, smallest / len(cuts), high / len(cuts))
        level = level * jnp.repeat(jnp.exp(steps), dims[dim] // blocks).reshape((-1,) + (1,) * (len(dims) - 1 - dim))
    return level


def scatter_about(own_key, extent, scale, most, split=(), kind=jnp.bfloat16):
    result = jax.random.normal(own_key, extent, jnp.float32) * scale
    if len(split) > 0:
        result = levels(own_key, extent, split, -0.22, 0.18) * result
    return jnp.clip(result, min=-most, max=most).astype(kind)


def heavy_noise(rng, shape, scale, bound, pieces, heavy, kind=jnp.bfloat16):
    entries = scale * jax.random.normal(rng, shape, jnp.float32)
    if pieces:
        entries = entries * levels(rng, shape, pieces, -0.22, 0.18)
    return jnp.clip(spiked(entries, jax.random.fold_in(rng, 3), *heavy), -bound, bound).astype(kind)


def setup_inputs(seed: int = 0) -> dict:
    keys = jax.random.split(jax.random.key(seed), 6)
    inputs = scatter_about(keys[0], (TOKENS, D), 1.0, 6.0, ((0, 8), (1, 4)))
    cotangent = heavy_noise(keys[1], (TOKENS, D), 1.0, 8.0, ((0, 8), (1, 4)), (0, 1, 8, 2.0))
    gate_weight = scatter_about(keys[2], (D, FF), D ** -0.5, 0.125, ((0, 8), (1, 4)))
    up_weight = scatter_about(keys[3], (D, FF), D ** -0.5, 0.125, ((0, 8), (1, 4)))
    down_weight = scatter_about(keys[4], (FF, D), FF ** -0.5, 0.078125, ((0, 4), (1, 8)))
    return {"inputs": inputs, "cotangent": cotangent, "gate_weight": gate_weight, "up_weight": up_weight, "down_weight": down_weight}


def contract_rows(left, right):
    return lax.dot_general(left, right, (((0,), (0,)), ((), ())), preferred_element_type=jnp.float32)


def contract_cols(left, right):
    return lax.dot_general(left, right, (((1,), (1,)), ((), ())), preferred_element_type=jnp.float32)


def reference(inputs, cotangent, gate_weight, up_weight, down_weight):
    gate_pre = jnp.dot(inputs, gate_weight, preferred_element_type=jnp.float32)
    up_pre = jnp.dot(inputs, up_weight, preferred_element_type=jnp.float32)
    gate_sig = jax.nn.sigmoid(gate_pre)
    gate_act = gate_pre * gate_sig
    hidden = (gate_act * up_pre).astype(jnp.bfloat16)
    grad_hidden = contract_cols(cotangent, down_weight)
    grad_gate_pre = (grad_hidden * up_pre * gate_sig * (1.0 + gate_pre * (1.0 - gate_sig))).astype(jnp.bfloat16)
    grad_up_pre = (grad_hidden * gate_act).astype(jnp.bfloat16)
    grad_gate = contract_rows(inputs, grad_gate_pre)
    grad_up = contract_rows(inputs, grad_up_pre)
    grad_down = contract_rows(hidden, cotangent)
    width = FF // N_TP

    def add_block(block_index, running):
        offset = (block_index * width).astype(jnp.int32)
        block_gate = lax.dynamic_slice_in_dim(grad_gate_pre, offset, width, 1)
        block_up = lax.dynamic_slice_in_dim(grad_up_pre, offset, width, 1)
        weight_gate = lax.dynamic_slice_in_dim(gate_weight, offset, width, 1)
        weight_up = lax.dynamic_slice_in_dim(up_weight, offset, width, 1)
        partial_sum = contract_cols(block_gate, weight_gate) + contract_cols(block_up, weight_up)
        rounded = lax.optimization_barrier(partial_sum.astype(jnp.bfloat16))
        return running + rounded.astype(jnp.float32)

    summed = lax.fori_loop(0, N_TP, add_block, jnp.zeros(inputs.shape, jnp.float32))
    grad_inputs = summed.astype(jnp.bfloat16)
    return (grad_inputs, grad_gate, grad_up, grad_down)
```

```python
import functools

import jax
import jax.numpy as jnp
from jax import lax
from jax.experimental import pallas as pl
from jax.experimental.pallas import tpu as pltpu
from jax.sharding import PartitionSpec as P

MESH = pl.DeviceIdType.MESH
ANY = pl.BlockSpec(memory_space=pl.ANY)
VMEM = pl.BlockSpec(memory_space=pltpu.VMEM)
CORES = 2


def contract_rows(left, right):
    return lax.dot_general(
        left, right, (((0,), (0,)), ((), ())), preferred_element_type=jnp.float32
    )


def contract_cols(left, right):
    return lax.dot_general(
        left, right, (((1,), (1,)), ((), ())), preferred_element_type=jnp.float32
    )


def gathered_plan(inputs, cotangent, gate_weight, up_weight, down_weight):
    whole_inputs = lax.all_gather(inputs, "tp", axis=1, tiled=True)
    whole_cotangent = lax.all_gather(cotangent, "tp", axis=1, tiled=True)
    gate_whole = lax.all_gather(gate_weight, "fs", axis=0, tiled=True)
    up_whole = lax.all_gather(up_weight, "fs", axis=0, tiled=True)
    down_whole = lax.all_gather(down_weight, "fs", axis=1, tiled=True)
    gate_pre = jnp.dot(whole_inputs, gate_whole, preferred_element_type=jnp.float32)
    up_pre = jnp.dot(whole_inputs, up_whole, preferred_element_type=jnp.float32)
    grad_hidden = contract_cols(whole_cotangent, down_whole)
    hidden, grad_gate_pre, grad_up_pre = pointwise(gate_pre, up_pre, grad_hidden)
    pre_grads = jnp.concatenate([grad_gate_pre, grad_up_pre], axis=1)
    width = gate_weight.shape[1]
    partial_sum = contract_cols(grad_gate_pre, gate_whole) + contract_cols(grad_up_pre, up_whole)

    def scattered(values, axis, dim):
        return lax.psum_scatter(
            values.astype(jnp.bfloat16), axis, scatter_dimension=dim, tiled=True
        )

    grad_inputs = scattered(partial_sum, "tp", 1)
    expand = scattered(contract_rows(whole_inputs, pre_grads), "fs", 0).astype(jnp.float32)
    down = scattered(contract_rows(whole_cotangent, hidden), "fs", 0).astype(jnp.float32)
    return (grad_inputs, expand[:, :width], expand[:, width:], down.T)


def pointwise(gate_pre, up_pre, grad_hidden):
    gate_sig = jax.nn.sigmoid(gate_pre)
    gate_act = gate_pre * gate_sig
    hidden = (gate_act * up_pre).astype(jnp.bfloat16)
    grad_gate_pre = (grad_hidden * up_pre * gate_sig * (1.0 + gate_pre * (1.0 - gate_sig))).astype(
        jnp.bfloat16
    )
    grad_up_pre = (grad_hidden * gate_act).astype(jnp.bfloat16)
    return hidden, grad_gate_pre, grad_up_pre


def block(index, size):
    return pl.ds(pl.multiple_of(index * size, size), size)


class Place:
    def __init__(self, nz, ny, nx):
        self.nz, self.ny, self.nx = nz, ny, nx
        fs, tp = lax.axis_index("fs"), lax.axis_index("tp")
        self.fs, self.tp = fs, tp
        self.z, self.y = fs // ny, fs % ny
        self.x, self.c = tp // CORES, tp % CORES

    def by_z(self, dz):
        return {"fs": ((self.z + dz) % self.nz) * self.ny + self.y, "tp": self.tp}

    def by_y(self, dy):
        return {"fs": self.z * self.ny + (self.y + dy) % self.ny, "tp": self.tp}

    def by_x(self, dx):
        return {"fs": self.fs, "tp": ((self.x + dx) % self.nx) * CORES + self.c}

    def by_core(self):
        return {"fs": self.fs, "tp": self.x * CORES + 1 - self.c}

    def by_tp(self, dt):
        return {"fs": self.fs, "tp": (self.tp + dt) % (self.nx * CORES)}


def meet(partners):
    barrier = pltpu.get_barrier_semaphore()
    for partner in partners:
        pl.semaphore_signal(barrier, inc=1, device_id=partner, device_id_type=MESH)
    pl.semaphore_wait(barrier, len(partners))


class Copies:
    def __init__(self, send_sem, recv_sem):
        self.send_sem, self.recv_sem, self.made = send_sem, recv_sem, []

    def start(self, source, target, device):
        at = len(self.made)
        copy = pltpu.make_async_remote_copy(
            src_ref=source, dst_ref=target, send_sem=self.send_sem.at[at],
            recv_sem=self.recv_sem.at[at], device_id=device, device_id_type=MESH,
        )
        copy.start()
        self.made.append(copy)
        return copy


def gather_kernel(sizes, x_ref, c_ref, w_ref, xf, cf, wf, send_sem, recv_sem, own_sem):
    nz, ny, nx = sizes
    me = Place(*sizes)
    tokens, features = x_ref.shape
    depth = w_ref.shape[3]
    meet(
        [me.by_z(d) for d in range(1, nz)]
        + [me.by_y(d) for d in range(1, ny)]
        + [me.by_x(d) for d in range(1, nx)]
        + [me.by_core()]
    )
    copies = Copies(send_sem, recv_sem)
    pairs = ((x_ref, xf), (c_ref, cf))

    def spot(whole, dz, tp):
        return whole.at[block((me.z - dz + nz) % nz, tokens), block(tp, features)]

    def w_spot(dz):
        return wf.at[:, :, block(((me.z - dz + nz) % nz) * ny + me.y, depth)]

    own = []
    for at, (source, target) in enumerate(
        [(source, spot(whole, 0, me.tp)) for source, whole in pairs]
        + [(w_ref.at[me.z], w_spot(0))]
    ):
        own.append(pltpu.make_async_copy(source, target, own_sem.at[at]))
        own[-1].start()
    across = {}
    sent_z = [
        [copies.start(source, spot(whole, 0, me.tp), me.by_z(dz)) for source, whole in pairs]
        for dz in range(1, nz)
    ]
    for dx in range(1, nx):
        across[0, dx] = [
            copies.start(source, spot(whole, 0, me.tp), me.by_x(dx)) for source, whole in pairs
        ]
    last = [copies.start(source, spot(whole, 0, me.tp), me.by_core()) for source, whole in pairs]
    w_sent = [
        copies.start(w_ref.at[(me.z + dz) % nz], w_spot(0), me.by_z(dz)) for dz in range(1, nz)
    ]
    last += [copies.start(w_ref.at[me.z], w_spot(0), me.by_y(dy)) for dy in range(1, ny)]
    for dz in range(1, nz):
        for copy in sent_z[dz - 1]:
            copy.wait_recv()
        for dx in range(1, nx):
            across[dz, dx] = [
                copies.start(spot(whole, dz, me.tp), spot(whole, dz, me.tp), me.by_x(dx))
                for _, whole in pairs
            ]
        last += [
            copies.start(spot(whole, dz, me.tp), spot(whole, dz, me.tp), me.by_core())
            for _, whole in pairs
        ]
    for dz in range(nz):
        if dz:
            w_sent[dz - 1].wait_recv()
            last += [copies.start(w_spot(dz), w_spot(dz), me.by_y(dy)) for dy in range(1, ny)]
        for dx in range(1, nx):
            for copy in across[dz, dx]:
                copy.wait_recv()
            tp = ((me.x - dx + nx) % nx) * CORES + me.c
            last += [
                copies.start(spot(whole, dz, tp), spot(whole, dz, tp), me.by_core())
                for _, whole in pairs
            ]
    for copy in last:
        copy.wait_recv()
    for copy in copies.made:
        copy.wait_send()
    for copy in own:
        copy.wait()


def spread_kernel(sizes, g_ref, i_ref, rg, ri, send_sem, recv_sem):
    nz, ny, nx = sizes
    me = Place(*sizes)
    n_tp = nx * CORES
    depth, features = rg.shape[3] // nz, ri.shape[2]
    meet([me.by_y(d) for d in range(1, ny)] + [me.by_tp(d) for d in range(1, n_tp)])
    copies = Copies(send_sem, recv_sem)
    for dy in range(1, ny):
        for z in range(nz):
            copies.start(
                g_ref.at[:, :, block(z * ny + (me.y + dy) % ny, depth)],
                rg.at[dy - 1, :, :, pl.ds(z * depth, depth)],
                me.by_y(dy),
            )
    for dt in range(1, n_tp):
        copies.start(
            i_ref.at[:, block((me.tp + dt) % n_tp, features)], ri.at[dt - 1], me.by_tp(dt)
        )
    for copy in copies.made:
        copy.wait()


def settle_kernel(sizes, s_ref, i_ref, r, rz, send_sem, recv_sem, own_sem):
    nz, _, _ = sizes
    me = Place(*sizes)
    depth, tokens, units = s_ref.shape[2] // nz, rz.shape[1], s_ref.shape[1]
    meet([me.by_z(d) for d in range(1, nz)])
    target = r.at[:, block(me.z, units), :]
    own = pltpu.make_async_copy(s_ref.at[:, :, block(me.z, depth)], target, own_sem)
    own.start()
    copies = Copies(send_sem, recv_sem)
    for dz in range(1, nz):
        there = (me.z + dz) % nz
        copies.start(s_ref.at[:, :, block(there, depth)], target, me.by_z(dz))
        copies.start(i_ref.at[block(there, tokens), :], rz.at[dz - 1], me.by_z(dz))
    for copy in copies.made:
        copy.wait()
    own.wait()


def call(kernel, sizes, shapes, in_specs, count, own, identity, *operands):
    semaphores = [pltpu.SemaphoreType.DMA((count,)), pltpu.SemaphoreType.DMA((count,))]
    return pl.pallas_call(
        functools.partial(kernel, sizes),
        out_shape=[jax.ShapeDtypeStruct(shape, jnp.bfloat16) for shape in shapes],
        in_specs=in_specs,
        out_specs=[ANY] * len(shapes),
        scratch_shapes=semaphores + own,
        compiler_params=pltpu.CompilerParams(collective_id=identity, has_side_effects=True),
    )(*operands)


def split_plan(sizes, inputs, cotangent, gate_weight, up_weight, down_weight):
    nz, ny, nx = sizes
    n_tp = nx * CORES
    tokens, features = inputs.shape
    depth, width = gate_weight.shape
    units, rows, model = width // nz, tokens * nz, depth * nz * ny
    here_z = lax.axis_index("fs") // ny
    here_y = lax.axis_index("fs") % ny
    here_tp = lax.axis_index("tp")
    weights = jnp.stack(
        [
            gate_weight.T.reshape(nz, units, depth),
            up_weight.T.reshape(nz, units, depth),
            down_weight.reshape(nz, units, depth),
        ],
        axis=1,
    )
    count = 2 * (nz * (nx - 1) + nz * nx + nz - 1) + nz - 1 + nz * (ny - 1)
    all_x, all_c, all_w = call(
        gather_kernel, sizes, [(rows, model), (rows, model), (3, units, model)],
        [VMEM] * 3, count, [pltpu.SemaphoreType.DMA((3,))], 0, inputs, cotangent, weights,
    )
    gate_pre = contract_cols(all_x, all_w[0])
    up_pre = contract_cols(all_x, all_w[1])
    grad_hidden = contract_cols(all_c, all_w[2])
    hidden, grad_gate_pre, grad_up_pre = pointwise(gate_pre, up_pre, grad_hidden)
    partial = jnp.dot(grad_gate_pre, all_w[0], preferred_element_type=jnp.float32) + jnp.dot(
        grad_up_pre, all_w[1], preferred_element_type=jnp.float32
    )
    partial = partial.astype(jnp.bfloat16)
    grads = jnp.stack(
        [
            contract_rows(grad_gate_pre, all_x).astype(jnp.bfloat16),
            contract_rows(grad_up_pre, all_x).astype(jnp.bfloat16),
            contract_rows(hidden, all_c).astype(jnp.bfloat16),
        ]
    )
    from_y, from_tp = call(
        spread_kernel, sizes, [(ny - 1, 3, units, nz * depth), (n_tp - 1, rows, features)],
        [ANY] * 2, nz * (ny - 1) + n_tp - 1, [], 1, grads, partial,
    )
    mine = lax.dynamic_index_in_dim(
        grads.reshape(3, units, nz, ny, depth), here_y, 3, keepdims=False
    ).reshape(3, units, nz * depth)
    summed = mine.astype(jnp.float32) + from_y.astype(jnp.float32).sum(0)
    part = lax.dynamic_slice_in_dim(partial, here_tp * features, features, 1)
    part = part.astype(jnp.float32) + from_tp.astype(jnp.float32).sum(0)
    part = part.astype(jnp.bfloat16)
    settled, from_z = call(
        settle_kernel, sizes, [(3, width, depth), (nz - 1, tokens, features)],
        [VMEM] * 2, 2 * (nz - 1), [pltpu.SemaphoreType.DMA], 2,
        summed.astype(jnp.bfloat16), part,
    )
    own = lax.dynamic_slice_in_dim(part, here_z * tokens, tokens, 0)
    grad_inputs = own.astype(jnp.float32) + from_z.astype(jnp.float32).sum(0)
    return (
        grad_inputs.astype(jnp.bfloat16),
        settled[0].T.astype(jnp.float32),
        settled[1].T.astype(jnp.float32),
        settled[2].astype(jnp.float32),
    )


def solution(mesh):
    n_fs, n_tp = mesh.shape["fs"], mesh.shape["tp"]
    nx = max(1, n_tp // CORES)
    ny = nx
    nz = n_fs // ny

    def per_device(inputs, cotangent, gate_weight, up_weight, down_weight):
        arrays = (inputs, cotangent, gate_weight, up_weight, down_weight)
        depth, width = gate_weight.shape
        fits = n_tp == nx * CORES and nz > 1 and ny > 1 and n_fs == nz * ny
        tiles = depth % 128 == 0 and inputs.shape[1] % 128 == 0 and inputs.shape[0] % 16 == 0
        if fits and tiles and width % (16 * nz) == 0:
            return split_plan((nz, ny, nx), *arrays)
        return gathered_plan(*arrays)

    return jax.shard_map(
        per_device,
        mesh=mesh,
        in_specs=(P("fs", "tp"), P("fs", "tp"), P("fs", "tp"), P("fs", "tp"), P("tp", "fs")),
        out_specs=(P("fs", "tp"), P("fs", "tp"), P("fs", "tp"), P("tp", "fs")),
        check_vma=False,
    )
```

```python
import functools

import jax
import jax.numpy as jnp
from jax import lax
from jax.experimental import pallas as pl
from jax.experimental.pallas import tpu as pltpu
from jax.sharding import PartitionSpec as P

MESH = pl.DeviceIdType.MESH
ANY = pl.BlockSpec(memory_space=pl.ANY)
VMEM = pl.BlockSpec(memory_space=pltpu.VMEM)
CORES = 2


def contract_rows(left, right):
    return lax.dot_general(
        left, right, (((0,), (0,)), ((), ())), preferred_element_type=jnp.float32
    )


def contract_cols(left, right):
    return lax.dot_general(
        left, right, (((1,), (1,)), ((), ())), preferred_element_type=jnp.float32
    )


def gathered_plan(inputs, cotangent, gate_weight, up_weight, down_weight):
    whole_inputs = lax.all_gather(inputs, "tp", axis=1, tiled=True)
    whole_cotangent = lax.all_gather(cotangent, "tp", axis=1, tiled=True)
    gate_whole = lax.all_gather(gate_weight, "fs", axis=0, tiled=True)
    up_whole = lax.all_gather(up_weight, "fs", axis=0, tiled=True)
    down_whole = lax.all_gather(down_weight, "fs", axis=1, tiled=True)
    gate_pre = jnp.dot(whole_inputs, gate_whole, preferred_element_type=jnp.float32)
    up_pre = jnp.dot(whole_inputs, up_whole, preferred_element_type=jnp.float32)
    grad_hidden = contract_cols(whole_cotangent, down_whole)
    hidden, grad_gate_pre, grad_up_pre = pointwise(gate_pre, up_pre, grad_hidden)
    pre_grads = jnp.concatenate([grad_gate_pre, grad_up_pre], axis=1)
    width = gate_weight.shape[1]
    partial_sum = contract_cols(grad_gate_pre, gate_whole) + contract_cols(grad_up_pre, up_whole)

    def scattered(values, axis, dim):
        return lax.psum_scatter(
            values.astype(jnp.bfloat16), axis, scatter_dimension=dim, tiled=True
        )

    grad_inputs = scattered(partial_sum, "tp", 1)
    expand = scattered(contract_rows(whole_inputs, pre_grads), "fs", 0).astype(jnp.float32)
    down = scattered(contract_rows(whole_cotangent, hidden), "fs", 0).astype(jnp.float32)
    return (grad_inputs, expand[:, :width], expand[:, width:], down.T)


def pointwise(gate_pre, up_pre, grad_hidden):
    gate_sig = jax.nn.sigmoid(gate_pre)
    gate_act = gate_pre * gate_sig
    hidden = (gate_act * up_pre).astype(jnp.bfloat16)
    grad_gate_pre = (grad_hidden * up_pre * gate_sig * (1.0 + gate_pre * (1.0 - gate_sig))).astype(
        jnp.bfloat16
    )
    grad_up_pre = (grad_hidden * gate_act).astype(jnp.bfloat16)
    return hidden, grad_gate_pre, grad_up_pre


def block(index, size):
    return pl.ds(pl.multiple_of(index * size, size), size)


class Place:
    def __init__(self, nz, ny, nx):
        self.nz, self.ny, self.nx = nz, ny, nx
        fs, tp = lax.axis_index("fs"), lax.axis_index("tp")
        self.fs, self.tp = fs, tp
        self.z, self.y = fs // ny, fs % ny
        self.x, self.c = tp // CORES, tp % CORES

    def by_z(self, dz):
        return {"fs": ((self.z + dz) % self.nz) * self.ny + self.y, "tp": self.tp}

    def by_y(self, dy):
        return {"fs": self.z * self.ny + (self.y + dy) % self.ny, "tp": self.tp}

    def by_x(self, dx):
        return {"fs": self.fs, "tp": ((self.x + dx) % self.nx) * CORES + self.c}

    def by_core(self):
        return {"fs": self.fs, "tp": self.x * CORES + 1 - self.c}

    def by_tp(self, dt):
        return {"fs": self.fs, "tp": (self.tp + dt) % (self.nx * CORES)}


def meet(partners):
    barrier = pltpu.get_barrier_semaphore()
    for partner in partners:
        pl.semaphore_signal(barrier, inc=1, device_id=partner, device_id_type=MESH)
    pl.semaphore_wait(barrier, len(partners))


class Copies:
    def __init__(self, send_sem, recv_sem):
        self.send_sem, self.recv_sem, self.made = send_sem, recv_sem, []

    def start(self, source, target, device):
        at = len(self.made)
        copy = pltpu.make_async_remote_copy(
            src_ref=source, dst_ref=target, send_sem=self.send_sem.at[at],
            recv_sem=self.recv_sem.at[at], device_id=device, device_id_type=MESH,
        )
        copy.start()
        self.made.append(copy)
        return copy


def flip(value, mask, nz):
    bit = 1
    while bit < nz:
        if mask & bit:
            value = value + bit - 2 * bit * ((value // bit) % 2)
        bit *= 2
    return value


def far_first(nz):
    return sorted(range(1, nz), key=lambda d: -min(d, nz - d))


def gather_kernel(sizes, x_ref, c_ref, *refs):
    nz, ny, nx = sizes
    me = Place(*sizes)
    w_refs, (xf, cf, *wfs) = refs[:3], refs[3:8]
    send_sem, recv_sem, own_sem = refs[8:]
    tokens, features = x_ref.shape
    depth, units = w_refs[0].shape[1], w_refs[0].shape[0] // nz
    bits = [1 << at for at in reversed(range(nz.bit_length() - 1))]
    meet(
        [me.by_z(d) for d in range(1, nz)]
        + [me.by_y(d) for d in range(1, ny)]
        + [me.by_x(d) for d in range(1, nx)]
        + [me.by_core()]
    )
    copies = Copies(send_sem, recv_sem)
    wholes = (xf, cf)
    by_x, sent_z, w_sent, last = {}, {}, {}, []

    def spot(whole, mask, tp):
        return whole.at[block(flip(me.z, mask, nz), tokens), block(tp, features)]

    def w_spot(whole, dz):
        return whole.at[:, block(((me.z - dz + nz) % nz) * ny + me.y, depth)]

    def held(mask):
        return (x_ref, c_ref) if mask == 0 else [spot(whole, mask, me.tp) for whole in wholes]

    def pass_z(bit, mask):
        there = {"fs": flip(me.z, bit, nz) * ny + me.y, "tp": me.tp}
        sent_z[bit, mask] = [
            copies.start(source, spot(whole, mask, me.tp), there)
            for source, whole in zip(held(mask), wholes)
        ]

    def pass_tp(mask):
        for dx in range(1, nx):
            by_x[mask, dx] = [
                copies.start(source, spot(whole, mask, me.tp), me.by_x(dx))
                for source, whole in zip(held(mask), wholes)
            ]
        for source, whole in zip(held(mask), wholes):
            last.append(copies.start(source, spot(whole, mask, me.tp), me.by_core()))

    def pass_core(mask):
        for dx in range(1, nx):
            tp = ((me.x - dx + nx) % nx) * CORES + me.c
            for copy, whole in zip(by_x[mask, dx], wholes):
                copy.wait_recv()
                here = spot(whole, mask, tp)
                last.append(copies.start(here, here, me.by_core()))

    def send_w(dz):
        w_sent[dz] = [
            copies.start(w.at[block((me.z + dz) % nz, units), :], w_spot(wf, 0), me.by_z(dz))
            for w, wf in zip(w_refs, wfs)
        ]

    for bit in bits:
        pass_z(bit, 0)
    pass_tp(0)
    order = far_first(nz)
    send_w(order[0])
    own = []
    for w, wf in zip(w_refs, wfs):
        mine = w.at[block(me.z, units), :]
        last += [copies.start(mine, w_spot(wf, 0), me.by_y(dy)) for dy in range(1, ny)]
        own.append((mine, w_spot(wf, 0)))
    own += [(x_ref, spot(xf, 0, me.tp)), (c_ref, spot(cf, 0, me.tp))]
    own = [pltpu.make_async_copy(*pair, own_sem.at[at]) for at, pair in enumerate(own)]
    for copy in own:
        copy.start()
    masks = [0]
    for at, bit in enumerate(bits):
        for mask in list(masks):
            for copy in sent_z[bit, mask]:
                copy.wait_recv()
            masks.append(mask + bit)
            for lower in bits[at + 1 :]:
                pass_z(lower, mask + bit)
            pass_tp(mask + bit)
        if at == 0:
            for dz in order[1:]:
                send_w(dz)
    for at, dz in enumerate(order):
        for copy, wf in zip(w_sent[dz], wfs):
            copy.wait_recv()
            here = w_spot(wf, dz)
            last += [copies.start(here, here, me.by_y(dy)) for dy in range(1, ny)]
        pass_core(masks[at])
    pass_core(masks[-1])
    for copy in last:
        copy.wait_recv()
    for copy in copies.made:
        copy.wait_send()
    for copy in own:
        copy.wait()


def reduce_kernel(sizes, *refs):
    nz, ny, nx = sizes
    me = Place(*sizes)
    n_tp = nx * CORES
    g_refs, i_ref, r, out = refs[:3], refs[3], refs[4], refs[5]
    rg, sg, ri, si, rz, send_sem, recv_sem, own_sem = refs[6:]
    units, depth = rg.shape[3:]
    tokens, features = rz.shape[1:]
    meet(
        [me.by_y(d) for d in range(1, ny)]
        + [me.by_tp(d) for d in range(1, n_tp)]
        + [me.by_z(d) for d in range(1, nz)]
    )
    copies = Copies(send_sem, recv_sem)
    order = far_first(nz) + [0]
    by_y, by_tp = {}, {}
    for dz in order:
        there = (me.z + dz) % nz
        for at, g in enumerate(g_refs):
            by_y[dz, at] = [
                copies.start(
                    g.at[:, block(there * ny + (me.y + dy) % ny, depth)],
                    rg.at[dy - 1, dz, at],
                    me.by_y(dy),
                )
                for dy in range(1, ny)
            ]
        by_tp[dz] = [
            copies.start(
                i_ref.at[block(there, tokens), block((me.tp + dt) % n_tp, features)],
                ri.at[dt - 1, dz],
                me.by_tp(dt),
            )
            for dt in range(1, n_tp)
        ]
    final, waiting = [], []

    def release():
        while waiting:
            final.append(copies.start(*waiting.pop(0)))

    for dz in order:
        there = (me.z + dz) % nz
        for at, g in enumerate(g_refs):
            total = g[:, block(there * ny + me.y, depth)].astype(jnp.float32)
            for dy, copy in enumerate(by_y[dz, at]):
                copy.wait_recv()
                total += rg[dy, dz, at].astype(jnp.float32)
            sg[dz, at] = total.astype(jnp.bfloat16)
            release()
            if dz:
                target = r.at[at, block(me.z, units), :]
                waiting.append((sg.at[dz, at], target, me.by_z(dz)))
    for dz in order:
        rows = block((me.z + dz) % nz, tokens)
        total = i_ref[rows, block(me.tp, features)].astype(jnp.float32)
        for dt, copy in enumerate(by_tp[dz]):
            copy.wait_recv()
            total += ri[dt, dz].astype(jnp.float32)
        si[dz] = total.astype(si.dtype)
        release()
        if dz:
            waiting.append((si.at[dz], rz.at[dz - 1], me.by_z(dz)))
    own = pltpu.make_async_copy(sg.at[0], r.at[:, block(me.z, units), :], own_sem)
    own.start()
    for copy in final:
        copy.wait_recv()
    total = si[0].astype(jnp.float32)
    for dz in range(1, nz):
        total += rz[dz - 1].astype(jnp.float32)
    out[...] = total.astype(out.dtype)
    for copy in copies.made:
        copy.wait_send()
    own.wait()


def split_plan(sizes, inputs, cotangent, gate_weight, up_weight, down_weight):
    nz, ny, nx = sizes
    n_tp = nx * CORES
    tokens, features = inputs.shape
    depth, width = gate_weight.shape
    units, rows, model = width // nz, tokens * nz, depth * nz * ny
    dma, half = pltpu.SemaphoreType.DMA, jnp.bfloat16
    count = 2 * (nz * (nx - 1) + nz * nx + nz - 1) + 3 * (nz - 1) + 3 * nz * (ny - 1)
    all_x, all_c, gate_whole, up_whole, down_whole = pl.pallas_call(
        functools.partial(gather_kernel, sizes),
        out_shape=[jax.ShapeDtypeStruct((rows, model), half)] * 2
        + [jax.ShapeDtypeStruct((units, model), half)] * 3,
        in_specs=[VMEM] * 5,
        out_specs=[ANY] * 5,
        scratch_shapes=[dma((count,)), dma((count,)), dma((5,))],
        compiler_params=pltpu.CompilerParams(collective_id=0, has_side_effects=True),
    )(inputs, cotangent, gate_weight.T, up_weight.T, down_weight)
    gate_pre = contract_cols(all_x, gate_whole)
    up_pre = contract_cols(all_x, up_whole)
    grad_hidden = contract_cols(all_c, down_whole)
    hidden, grad_gate_pre, grad_up_pre = pointwise(gate_pre, up_pre, grad_hidden)
    partial = jnp.dot(grad_gate_pre, gate_whole, preferred_element_type=jnp.float32) + jnp.dot(
        grad_up_pre, up_whole, preferred_element_type=jnp.float32
    )
    count = nz * (3 * (ny - 1) + n_tp - 1) + 4 * (nz - 1)
    settled, grad_inputs = pl.pallas_call(
        functools.partial(reduce_kernel, sizes),
        out_shape=[
            jax.ShapeDtypeStruct((3, width, depth), half),
            jax.ShapeDtypeStruct((tokens, features), half),
        ],
        in_specs=[VMEM] * 4,
        out_specs=[ANY, VMEM],
        scratch_shapes=[
            pltpu.VMEM((ny - 1, nz, 3, units, depth), half),
            pltpu.VMEM((nz, 3, units, depth), half),
            pltpu.VMEM((n_tp - 1, nz, tokens, features), half),
            pltpu.VMEM((nz, tokens, features), half),
            pltpu.VMEM((nz - 1, tokens, features), half),
            dma((count,)),
            dma((count,)),
            dma,
        ],
        compiler_params=pltpu.CompilerParams(collective_id=1, has_side_effects=True),
    )(
        contract_rows(grad_gate_pre, all_x).astype(half),
        contract_rows(grad_up_pre, all_x).astype(half),
        contract_rows(hidden, all_c).astype(half),
        partial.astype(half),
    )
    return (
        grad_inputs,
        settled[0].T.astype(jnp.float32),
        settled[1].T.astype(jnp.float32),
        settled[2].astype(jnp.float32),
    )


def solution(mesh):
    n_fs, n_tp = mesh.shape["fs"], mesh.shape["tp"]
    nx = max(1, n_tp // CORES)
    ny = nx
    nz = n_fs // ny

    def per_device(inputs, cotangent, gate_weight, up_weight, down_weight):
        arrays = (inputs, cotangent, gate_weight, up_weight, down_weight)
        depth, width = gate_weight.shape
        fits = n_tp == nx * CORES and nz > 1 and ny > 1 and n_fs == nz * ny
        fits = fits and nz & (nz - 1) == 0
        tiles = depth % 128 == 0 and inputs.shape[1] % 128 == 0 and inputs.shape[0] % 16 == 0
        if fits and tiles and width % (16 * nz) == 0:
            return split_plan((nz, ny, nx), *arrays)
        return gathered_plan(*arrays)

    return jax.shard_map(
        per_device,
        mesh=mesh,
        in_specs=(P("fs", "tp"), P("fs", "tp"), P("fs", "tp"), P("fs", "tp"), P("tp", "fs")),
        out_specs=(P("fs", "tp"), P("fs", "tp"), P("fs", "tp"), P("tp", "fs")),
        check_vma=False,
    )
```

```python
import functools

import jax
import jax.numpy as jnp
from jax import lax
from jax.experimental import pallas as pl
from jax.experimental.pallas import tpu as pltpu
from jax.sharding import PartitionSpec as P

MESH = pl.DeviceIdType.MESH
ANY = pl.BlockSpec(memory_space=pl.ANY)
VMEM = pl.BlockSpec(memory_space=pltpu.VMEM)
CORES = 2


def contract_rows(left, right):
    return lax.dot_general(
        left, right, (((0,), (0,)), ((), ())), preferred_element_type=jnp.float32
    )


def contract_cols(left, right):
    return lax.dot_general(
        left, right, (((1,), (1,)), ((), ())), preferred_element_type=jnp.float32
    )


def gathered_plan(inputs, cotangent, gate_weight, up_weight, down_weight):
    whole_inputs = lax.all_gather(inputs, "tp", axis=1, tiled=True)
    whole_cotangent = lax.all_gather(cotangent, "tp", axis=1, tiled=True)
    gate_whole = lax.all_gather(gate_weight, "fs", axis=0, tiled=True)
    up_whole = lax.all_gather(up_weight, "fs", axis=0, tiled=True)
    down_whole = lax.all_gather(down_weight, "fs", axis=1, tiled=True)
    gate_pre = jnp.dot(whole_inputs, gate_whole, preferred_element_type=jnp.float32)
    up_pre = jnp.dot(whole_inputs, up_whole, preferred_element_type=jnp.float32)
    grad_hidden = contract_cols(whole_cotangent, down_whole)
    hidden, grad_gate_pre, grad_up_pre = pointwise(gate_pre, up_pre, grad_hidden)
    pre_grads = jnp.concatenate([grad_gate_pre, grad_up_pre], axis=1)
    width = gate_weight.shape[1]
    partial_sum = contract_cols(grad_gate_pre, gate_whole) + contract_cols(grad_up_pre, up_whole)

    def scattered(values, axis, dim):
        return lax.psum_scatter(
            values.astype(jnp.bfloat16), axis, scatter_dimension=dim, tiled=True
        )

    grad_inputs = scattered(partial_sum, "tp", 1)
    expand = scattered(contract_rows(whole_inputs, pre_grads), "fs", 0).astype(jnp.float32)
    down = scattered(contract_rows(whole_cotangent, hidden), "fs", 0).astype(jnp.float32)
    return (grad_inputs, expand[:, :width], expand[:, width:], down.T)


def pointwise(gate_pre, up_pre, grad_hidden):
    gate_sig = jax.nn.sigmoid(gate_pre)
    gate_act = gate_pre * gate_sig
    hidden = (gate_act * up_pre).astype(jnp.bfloat16)
    grad_gate_pre = (grad_hidden * up_pre * gate_sig * (1.0 + gate_pre * (1.0 - gate_sig))).astype(
        jnp.bfloat16
    )
    grad_up_pre = (grad_hidden * gate_act).astype(jnp.bfloat16)
    return hidden, grad_gate_pre, grad_up_pre


def block(index, size):
    return pl.ds(pl.multiple_of(index * size, size), size)


class Place:
    def __init__(self, nz, ny, nx):
        self.nz, self.ny, self.nx = nz, ny, nx
        fs, tp = lax.axis_index("fs"), lax.axis_index("tp")
        self.fs, self.tp = fs, tp
        self.z, self.y = fs // ny, fs % ny
        self.x, self.c = tp // CORES, tp % CORES

    def by_z(self, dz):
        return {"fs": ((self.z + dz) % self.nz) * self.ny + self.y, "tp": self.tp}

    def by_y(self, dy):
        return {"fs": self.z * self.ny + (self.y + dy) % self.ny, "tp": self.tp}

    def by_x(self, dx):
        return {"fs": self.fs, "tp": ((self.x + dx) % self.nx) * CORES + self.c}

    def by_core(self):
        return {"fs": self.fs, "tp": self.x * CORES + 1 - self.c}

    def by_tp(self, dt):
        return {"fs": self.fs, "tp": (self.tp + dt) % (self.nx * CORES)}


def meet(partners):
    barrier = pltpu.get_barrier_semaphore()
    for partner in partners:
        pl.semaphore_signal(barrier, inc=1, device_id=partner, device_id_type=MESH)
    pl.semaphore_wait(barrier, len(partners))


class Copies:
    def __init__(self, send_sem, recv_sem):
        self.send_sem, self.recv_sem, self.made = send_sem, recv_sem, []

    def start(self, source, target, device):
        at = len(self.made)
        copy = pltpu.make_async_remote_copy(
            src_ref=source, dst_ref=target, send_sem=self.send_sem.at[at],
            recv_sem=self.recv_sem.at[at], device_id=device, device_id_type=MESH,
        )
        copy.start()
        self.made.append(copy)
        return copy


def flip(value, mask, nz):
    bit = 1
    while bit < nz:
        if mask & bit:
            value = value + bit - 2 * bit * ((value // bit) % 2)
        bit *= 2
    return value


def far_first(nz):
    return sorted(range(1, nz), key=lambda d: -min(d, nz - d))


def gather_kernel(sizes, x_ref, c_ref, *refs):
    nz, ny, nx = sizes
    me = Place(*sizes)
    w_refs, (xf, cf, *wfs) = refs[:3], refs[3:8]
    send_sem, recv_sem, own_sem = refs[8:]
    tokens, features = x_ref.shape
    depth, units = w_refs[0].shape[1], w_refs[0].shape[0] // nz
    bits = [1 << at for at in reversed(range(nz.bit_length() - 1))]
    meet(
        [me.by_z(d) for d in range(1, nz)]
        + [me.by_y(d) for d in range(1, ny)]
        + [me.by_x(d) for d in range(1, nx)]
        + [me.by_core()]
    )
    copies = Copies(send_sem, recv_sem)
    wholes = (xf, cf)
    by_x, sent_z, w_sent, last = {}, {}, {}, []

    def spot(whole, mask, tp):
        return whole.at[block(flip(me.z, mask, nz), tokens), block(tp, features)]

    def w_spot(whole, dz):
        return whole.at[:, block(((me.z - dz + nz) % nz) * ny + me.y, depth)]

    def held(mask):
        return (x_ref, c_ref) if mask == 0 else [spot(whole, mask, me.tp) for whole in wholes]

    def pass_z(bit, mask):
        there = {"fs": flip(me.z, bit, nz) * ny + me.y, "tp": me.tp}
        sent_z[bit, mask] = [
            copies.start(source, spot(whole, mask, me.tp), there)
            for source, whole in zip(held(mask), wholes)
        ]

    def pass_tp(mask):
        for dx in range(1, nx):
            by_x[mask, dx] = [
                copies.start(source, spot(whole, mask, me.tp), me.by_x(dx))
                for source, whole in zip(held(mask), wholes)
            ]
        for source, whole in zip(held(mask), wholes):
            last.append(copies.start(source, spot(whole, mask, me.tp), me.by_core()))

    def pass_core(mask):
        for dx in range(1, nx):
            tp = ((me.x - dx + nx) % nx) * CORES + me.c
            for copy, whole in zip(by_x[mask, dx], wholes):
                copy.wait_recv()
                here = spot(whole, mask, tp)
                last.append(copies.start(here, here, me.by_core()))

    def send_w(dz):
        w_sent[dz] = [
            copies.start(w.at[block((me.z + dz) % nz, units), :], w_spot(wf, 0), me.by_z(dz))
            for w, wf in zip(w_refs, wfs)
        ]

    for bit in bits:
        pass_z(bit, 0)
    pass_tp(0)
    order = far_first(nz)
    send_w(order[0])
    own = []
    for w, wf in zip(w_refs, wfs):
        mine = w.at[block(me.z, units), :]
        last += [copies.start(mine, w_spot(wf, 0), me.by_y(dy)) for dy in range(1, ny)]
        own.append((mine, w_spot(wf, 0)))
    own += [(x_ref, spot(xf, 0, me.tp)), (c_ref, spot(cf, 0, me.tp))]
    own = [pltpu.make_async_copy(*pair, own_sem.at[at]) for at, pair in enumerate(own)]
    for copy in own:
        copy.start()
    masks = [0]
    for at, bit in enumerate(bits):
        for mask in list(masks):
            for copy in sent_z[bit, mask]:
                copy.wait_recv()
            masks.append(mask + bit)
            for lower in bits[at + 1 :]:
                pass_z(lower, mask + bit)
            pass_tp(mask + bit)
        if at == 0:
            for dz in order[1:]:
                send_w(dz)
    for at, dz in enumerate(order):
        for copy, wf in zip(w_sent[dz], wfs):
            copy.wait_recv()
            here = w_spot(wf, dz)
            last += [copies.start(here, here, me.by_y(dy)) for dy in range(1, ny)]
        pass_core(masks[at])
    pass_core(masks[-1])
    for copy in last:
        copy.wait_recv()
    for copy in copies.made:
        copy.wait_send()
    for copy in own:
        copy.wait()


def reduce_kernel(sizes, *refs):
    nz, ny, nx = sizes
    me = Place(*sizes)
    n_tp = nx * CORES
    g_refs, i_ref, r, out = refs[:3], refs[3], refs[4], refs[5]
    rg, sg, ri, si, rz, send_sem, recv_sem, own_sem = refs[6:]
    units, depth = rg.shape[3:]
    tokens, features = rz.shape[1:]
    meet(
        [me.by_y(d) for d in range(1, ny)]
        + [me.by_tp(d) for d in range(1, n_tp)]
        + [me.by_z(d) for d in range(1, nz)]
    )
    copies = Copies(send_sem, recv_sem)
    order = far_first(nz) + [0]
    by_y, by_tp = {}, {}
    for dz in order:
        there = (me.z + dz) % nz
        for at, g in enumerate(g_refs):
            by_y[dz, at] = [
                copies.start(
                    g.at[:, block(there * ny + (me.y + dy) % ny, depth)],
                    rg.at[dy - 1, dz, at],
                    me.by_y(dy),
                )
                for dy in range(1, ny)
            ]
    masks = sorted(range(nz), key=lambda m: m % 2 == 0)
    for mask in masks:
        by_tp[mask] = [
            copies.start(
                i_ref.at[block(flip(me.z, mask, nz), tokens), block((me.tp + dt) % n_tp, features)],
                ri.at[dt - 1, mask],
                me.by_tp(dt),
            )
            for dt in range(1, n_tp)
        ]
    final, waiting = [], []

    def release():
        while waiting:
            final.append(copies.start(*waiting.pop(0)))

    for dz in order:
        there = (me.z + dz) % nz
        for at, g in enumerate(g_refs):
            total = g[:, block(there * ny + me.y, depth)].astype(jnp.float32)
            for dy, copy in enumerate(by_y[dz, at]):
                copy.wait_recv()
                total += rg[dy, dz, at].astype(jnp.float32)
            sg[dz, at] = total.astype(jnp.bfloat16)
            release()
            if dz:
                target = r.at[at, block(me.z, units), :]
                waiting.append((sg.at[dz, at], target, me.by_z(dz)))
    release()
    own = pltpu.make_async_copy(sg.at[0], r.at[:, block(me.z, units), :], own_sem)
    own.start()
    halves, slots = {}, iter(range(nz - 1))

    def send_half(bit, mask):
        there = {"fs": flip(me.z, bit, nz) * ny + me.y, "tp": me.tp}
        slot = next(slots)
        halves[bit, mask - bit] = slot, copies.start(si.at[mask], rz.at[slot], there)

    for mask in masks:
        total = i_ref[block(flip(me.z, mask, nz), tokens), block(me.tp, features)]
        total = total.astype(jnp.float32)
        for dt, copy in enumerate(by_tp[mask]):
            copy.wait_recv()
            total += ri[dt, mask].astype(jnp.float32)
        si[mask] = total.astype(si.dtype)
    bit = 1
    while bit < nz:
        live = range(0, nz, bit)
        for mask in live:
            if mask & bit:
                send_half(bit, mask)
        for mask in sorted(live, key=lambda m: -(m & (2 * bit))):
            if mask & bit == 0:
                slot, copy = halves[bit, mask]
                copy.wait_recv()
                total = si[mask].astype(jnp.float32) + rz[slot].astype(jnp.float32)
                si[mask] = total.astype(si.dtype)
        bit *= 2
    out[...] = si[0]
    for copy in final:
        copy.wait_recv()
    for copy in copies.made:
        copy.wait_send()
    own.wait()


def split_plan(sizes, inputs, cotangent, gate_weight, up_weight, down_weight):
    nz, ny, nx = sizes
    n_tp = nx * CORES
    tokens, features = inputs.shape
    depth, width = gate_weight.shape
    units, rows, model = width // nz, tokens * nz, depth * nz * ny
    dma, half = pltpu.SemaphoreType.DMA, jnp.bfloat16
    count = 2 * (nz * (nx - 1) + nz * nx + nz - 1) + 3 * (nz - 1) + 3 * nz * (ny - 1)
    all_x, all_c, gate_whole, up_whole, down_whole = pl.pallas_call(
        functools.partial(gather_kernel, sizes),
        out_shape=[jax.ShapeDtypeStruct((rows, model), half)] * 2
        + [jax.ShapeDtypeStruct((units, model), half)] * 3,
        in_specs=[VMEM] * 5,
        out_specs=[ANY] * 5,
        scratch_shapes=[dma((count,)), dma((count,)), dma((5,))],
        compiler_params=pltpu.CompilerParams(collective_id=0, has_side_effects=True),
    )(inputs, cotangent, gate_weight.T, up_weight.T, down_weight)
    gate_pre = contract_cols(all_x, gate_whole)
    up_pre = contract_cols(all_x, up_whole)
    grad_hidden = contract_cols(all_c, down_whole)
    hidden, grad_gate_pre, grad_up_pre = pointwise(gate_pre, up_pre, grad_hidden)
    partial = jnp.dot(grad_gate_pre, gate_whole, preferred_element_type=jnp.float32) + jnp.dot(
        grad_up_pre, up_whole, preferred_element_type=jnp.float32
    )
    count = nz * (3 * (ny - 1) + n_tp - 1) + 4 * (nz - 1)
    settled, grad_inputs = pl.pallas_call(
        functools.partial(reduce_kernel, sizes),
        out_shape=[
            jax.ShapeDtypeStruct((3, width, depth), half),
            jax.ShapeDtypeStruct((tokens, features), half),
        ],
        in_specs=[VMEM] * 4,
        out_specs=[ANY, VMEM],
        scratch_shapes=[
            pltpu.VMEM((ny - 1, nz, 3, units, depth), half),
            pltpu.VMEM((nz, 3, units, depth), half),
            pltpu.VMEM((n_tp - 1, nz, tokens, features), half),
            pltpu.VMEM((nz, tokens, features), half),
            pltpu.VMEM((nz - 1, tokens, features), half),
            dma((count,)),
            dma((count,)),
            dma,
        ],
        compiler_params=pltpu.CompilerParams(collective_id=1, has_side_effects=True),
    )(
        contract_rows(grad_gate_pre, all_x).astype(half),
        contract_rows(grad_up_pre, all_x).astype(half),
        contract_rows(hidden, all_c).astype(half),
        partial.astype(half),
    )
    return (
        grad_inputs,
        settled[0].T.astype(jnp.float32),
        settled[1].T.astype(jnp.float32),
        settled[2].astype(jnp.float32),
    )


def solution(mesh):
    n_fs, n_tp = mesh.shape["fs"], mesh.shape["tp"]
    nx = max(1, n_tp // CORES)
    ny = nx
    nz = n_fs // ny

    def per_device(inputs, cotangent, gate_weight, up_weight, down_weight):
        arrays = (inputs, cotangent, gate_weight, up_weight, down_weight)
        depth, width = gate_weight.shape
        fits = n_tp == nx * CORES and nz > 1 and ny > 1 and n_fs == nz * ny
        fits = fits and nz & (nz - 1) == 0
        tiles = depth % 128 == 0 and inputs.shape[1] % 128 == 0 and inputs.shape[0] % 16 == 0
        if fits and tiles and width % (16 * nz) == 0:
            return split_plan((nz, ny, nx), *arrays)
        return gathered_plan(*arrays)

    return jax.shard_map(
        per_device,
        mesh=mesh,
        in_specs=(P("fs", "tp"), P("fs", "tp"), P("fs", "tp"), P("fs", "tp"), P("tp", "fs")),
        out_specs=(P("fs", "tp"), P("fs", "tp"), P("fs", "tp"), P("tp", "fs")),
        check_vma=False,
    )
```
